256 devices in a mesh: kv: 32 (over z, x), tp: 8 (over y, core).
Axes of the slice: x: 4, y: 4, z: 8, core: 2. Of those that a mesh axis runs over, the one named last changes fastest.
Arguments:
- tokens: bfloat16 [22, 4096], P(None, ('kv', 'tp')), may hold values from -22 to 22
- attn_gain: float32 [4096], P('kv'), may hold values from 0.1 to 1.9
- w_query: bfloat16 [4096, 4096], P('kv', 'tp'), may hold values from -0.09375 to 0.09375
- w_key: bfloat16 [4096, 4096], P('kv', 'tp'), may hold values from -0.5 to 0.5
- w_value: bfloat16 [4096, 4096], P('kv', 'tp'), may hold values from -0.09375 to 0.09375
- cache_keys: bfloat16 [22, 8192, 32, 128], P(None, 'kv', 'tp'), may hold values from -256 to 256
- cache_values: bfloat16 [22, 8192, 32, 128], P(None, 'kv', 'tp'), may hold values from -6 to 6
- lambdas: float32 [32], P('tp'), may hold values from 0.3 to 0.8
- head_gain: float32 [128], replicated, may hold values from 0.1 to 1.9
- w_out: bfloat16 [4096, 4096], P('tp', 'kv'), may hold values from -0.09375 to 0.09375
- mlp_gain: float32 [4096], P('kv'), may hold values from 0.1 to 1.9
- w_gate: bfloat16 [4096, 11008], P('kv', 'tp'), may hold values from -0.09375 to 0.09375
- w_up: bfloat16 [4096, 11008], P('kv', 'tp'), may hold values from -0.09375 to 0.09375
- w_down: bfloat16 [11008, 4096], P('tp', 'kv'), may hold values from -0.0546875 to 0.0546875
Outputs:
- output: bfloat16 [22, 4096], P(None, ('kv', 'tp'))
The draws below stay inside these ranges and needn't reach their ends.
All inputs are finite; a program needn't handle non-finite values.
Results may differ from the reference program's by a relative error of at most 0.017.
The reference program's roundings to bfloat16 on the way (of `normed_in`, `query_all`, `heads_out`, `residual`, `normed_mid` and `hidden`) count: a program that leaves them out, or rounds other values in their place, can miss the bound.
Values may be sent and summed in bfloat16 or wider, within the bound.
A program may use at most 64 MiB of HBM per device.

```python
import jax
import jax.numpy as jnp
from jax import lax

D = 4096
HEADS = 32
HEAD_DIM = 128
HALF = 64
FF = 11008
SEQS = 22
POS_DEV = 256
CACHE_LEN = 8192
N_KV = 32
N_TP = 8


def draw_tokens(key, part):
    key_base = jax.random.fold_in(key, 11)
    key_rows = jax.random.fold_in(key, 12)
    columns = jnp.arange(D, dtype=jnp.float32) / (D - 1)
    base_vals = jnp.clip(jax.random.normal(key_base, (SEQS, D), jnp.float32), -4.0, 4.0)
    col_scale = jnp.exp(jnp.log(3.0) * (columns - 0.5))
    row_scale = jnp.exp(jax.random.uniform(key_rows, (SEQS, 1), jnp.float32, jnp.log(1.0 / 3.0), jnp.log(3.0)))
    return (base_vals * row_scale * col_scale[None, :]).astype(jnp.bfloat16)


def draw_cache_keys(key, part):
    key_base = jax.random.fold_in(key, 21)
    base_vals = jnp.clip(jax.random.normal(key_base, (SEQS, CACHE_LEN, HEADS, HEAD_DIM), jnp.float32), -6.0, 6.0) * 1.75
    return base_vals.astype(jnp.bfloat16)


def block_levels(rng, shape, cuts, low, high):
    loudness, own = 1.0, jax.random.fold_in(rng, 6)
    for axis_at, blocks in cuts:
        steps = jnp.exp(jax.random.uniform(jax.random.fold_in(own, axis_at), (blocks,), jnp.float32, low / len(cuts), high / len(cuts)))
        loudness = loudness * jnp.repeat(steps, shape[axis_at] // blocks).reshape([-1 if axis == axis_at else 1 for axis in range(len(shape))])
    return loudness


def bell_draw(key, dims, spread, bound, split=(), kind=jnp.bfloat16):
    level = block_levels(key, dims, split, -0.22, 0.18) if split else 1.0
    entries = jax.random.normal(key, dims, jnp.float32) * spread * level
    return jnp.minimum(jnp.maximum(entries, -bound), bound).astype(kind)


def setup_inputs(seed: int = 0) -> dict:
    key_of = jax.random.split(jax.random.key(seed), 15)
    tokens = draw_tokens(jax.random.fold_in(key_of[14], 71), 0)
    attn_gain = jnp.clip(1.0 + 0.18 * jax.random.normal(key_of[1], (D,), jnp.float32), 0.1, 1.9)
    w_query = bell_draw(key_of[2], (D, HEADS * HEAD_DIM), D ** -0.5, 0.09375, ((0, 32), (1, 8)))
    w_key = bell_draw(key_of[3], (D, HEADS * HEAD_DIM), (D // 36) ** -0.5, 0.5, ((0, 32), (1, 8)))
    w_value = bell_draw(key_of[4], (D, HEADS * HEAD_DIM), D ** -0.5, 0.09375, ((0, 32), (1, 8)))
    cache_keys = draw_cache_keys(jax.random.fold_in(key_of[14], 71), 0)
    cache_values = bell_draw(key_of[6], (SEQS, CACHE_LEN, HEADS, HEAD_DIM), 1.0, 6.0, ((1, 32), (2, 8)))
    lambdas = jnp.clip(0.3 + 0.5 * jax.random.uniform(key_of[7], (HEADS,), jnp.float32) ** block_levels(key_of[7], (HEADS,), ((0, 8),), -0.2, 0.2), 0.3, 0.8)
    head_gain = jnp.clip(1.0 + 0.18 * jax.random.normal(key_of[8], (HEAD_DIM,), jnp.float32), 0.1, 1.9)
    w_out = bell_draw(key_of[9], (HEADS * HEAD_DIM, D), (HEADS * HEAD_DIM) ** -0.5, 0.09375, ((0, 8), (1, 32)))
    mlp_gain = jnp.clip(1.0 + 0.18 * jax.random.normal(key_of[10], (D,), jnp.float32), 0.1, 1.9)
    w_gate = bell_draw(key_of[11], (D, FF), D ** -0.5, 0.09375, ((0, 32), (1, 8)))
    w_up = bell_draw(key_of[12], (D, FF), D ** -0.5, 0.09375, ((0, 32), (1, 8)))
    w_down = bell_draw(key_of[13], (FF, D), FF ** -0.5, 0.0546875, ((0, 8), (1, 32)))
    return dict(tokens=tokens, attn_gain=attn_gain, w_query=w_query, w_key=w_key, w_value=w_value, cache_keys=cache_keys, cache_values=cache_values, lambdas=lambdas, head_gain=head_gain, w_out=w_out, mlp_gain=mlp_gain, w_gate=w_gate, w_up=w_up, w_down=w_down)


epsilon = 1e-06

def blocked_attention(query_vec, key_new, value_new, keys_head, values_head, low, high):
    seq_count = keys_head.shape[0]
    score_scale = HALF ** (-0.5)
    query_part = query_vec[:, low:high].astype(jnp.float32)
    scores = jnp.einsum('sd,std->st', query_part, keys_head[:, :, low:high].astype(jnp.float32)) * score_scale
    score_new = lax.optimization_barrier(jnp.sum(query_part * key_new[:, low:high].astype(jnp.float32), axis=1)) * score_scale
    blocks = scores.reshape(seq_count, N_KV, POS_DEV)
    maxima = lax.optimization_barrier(jnp.max(blocks, axis=2))
    weights = jnp.exp(blocks - maxima[:, :, None])
    totals = lax.optimization_barrier(jnp.sum(weights, axis=2))
    rounded = lax.optimization_barrier(weights.astype(jnp.bfloat16)).astype(jnp.float32)
    blocked_values = values_head.astype(jnp.float32).reshape(seq_count, N_KV, POS_DEV, HEAD_DIM)
    sums = jnp.einsum('snt,sntd->snd', rounded, blocked_values)
    peak = jnp.maximum(lax.optimization_barrier(jnp.max(maxima, axis=1)), score_new)
    block_weight = jnp.exp(maxima - peak[:, None])
    new_weight = jnp.exp(score_new - peak)
    denominator = lax.optimization_barrier(jnp.sum(block_weight * totals, axis=1)) + new_weight
    numerator = lax.optimization_barrier(jnp.sum(block_weight[:, :, None] * sums, axis=1)) + new_weight[:, None] * value_new.astype(jnp.float32)
    return numerator / denominator[:, None]

def grouped_product(activations, weights_mat, groups):
    span_rows = weights_mat.shape[0] // groups
    result = jnp.zeros((activations.shape[0], weights_mat.shape[1]), jnp.float32)
    for block_index in range(groups):
        partial_value = jnp.dot(activations[:, block_index * span_rows:(block_index + 1) * span_rows], weights_mat[block_index * span_rows:(block_index + 1) * span_rows], preferred_element_type=jnp.float32)
        result = result + lax.optimization_barrier(partial_value.astype(jnp.bfloat16)).astype(jnp.float32)
    return result

def reference(tokens, attn_gain, w_query, w_key, w_value, cache_keys, cache_values, lambdas, head_gain, w_out, mlp_gain, w_gate, w_up, w_down):
    seq_count = tokens.shape[0]
    tokens_f = tokens.astype(jnp.float32)
    scale_in = lax.rsqrt(lax.optimization_barrier(jnp.mean(tokens_f * tokens_f, axis=1, keepdims=True)) + epsilon)
    normed_in = (tokens_f * attn_gain.astype(jnp.float32)).astype(jnp.bfloat16)

    def project(weight):
        product = jnp.dot(normed_in, weight, preferred_element_type=jnp.float32)
        return (scale_in * product).astype(jnp.bfloat16).reshape(seq_count, HEADS, HEAD_DIM)
    query_all = project(w_query)
    key_all = project(w_key)
    value_all = project(w_value)

    def one_head(head_index):
        keys_head = lax.dynamic_index_in_dim(cache_keys, head_index, 2, keepdims=False)
        values_head = lax.dynamic_index_in_dim(cache_values, head_index, 2, keepdims=False)
        query_vec = lax.dynamic_index_in_dim(query_all, head_index, 1, keepdims=False)
        key_new = lax.dynamic_index_in_dim(key_all, head_index, 1, keepdims=False)
        value_new = lax.dynamic_index_in_dim(value_all, head_index, 1, keepdims=False)
        first_map = blocked_attention(query_vec, key_new, value_new, keys_head, values_head, 0, HALF)
        second_map = blocked_attention(query_vec, key_new, value_new, keys_head, values_head, HALF, HEAD_DIM)
        return (first_map, second_map)
    first_map, second_map = lax.map(one_head, jnp.arange(HEADS, dtype=jnp.int32))
    difference = first_map - lambdas.astype(jnp.float32)[:, None, None] * second_map
    normed = difference * lax.rsqrt(lax.optimization_barrier(jnp.mean(difference * difference, axis=2, keepdims=True)) + epsilon)
    normed = normed * head_gain.astype(jnp.float32)
    heads_out = jnp.transpose(normed, (1, 0, 2)).reshape(seq_count, HEADS * HEAD_DIM).astype(jnp.bfloat16)
    branch = grouped_product(heads_out, w_out, N_TP)
    residual = (tokens_f + branch).astype(jnp.bfloat16)
    residual_f = residual.astype(jnp.float32)
    scale_mid = lax.rsqrt(lax.optimization_barrier(jnp.mean(residual_f * residual_f, axis=1, keepdims=True)) + epsilon)
    normed_mid = (residual_f * mlp_gain.astype(jnp.float32)).astype(jnp.bfloat16)
    gate = scale_mid * jnp.dot(normed_mid, w_gate, preferred_element_type=jnp.float32)
    up_val = scale_mid * jnp.dot(normed_mid, w_up, preferred_element_type=jnp.float32)
    hidden = (jax.nn.silu(gate) * up_val).astype(jnp.bfloat16)
    mixer = grouped_product(hidden, w_down, N_TP)
    return (residual_f + mixer).astype(jnp.bfloat16)
```

```python
import functools

import jax
import jax.numpy as jnp
from jax import lax
from jax.experimental import pallas as pl
from jax.experimental.pallas import tpu as pltpu
from jax.sharding import PartitionSpec as P

MESH = pl.DeviceIdType.MESH
F32, BF16 = jnp.float32, jnp.bfloat16
D = 4096
EPS = 1e-06
ROWS = 24
SEQS = 22
N_KV, N_X, N_TP = 32, 4, 8
HEADS = 4
CHUNKS = 11
LOW = -3.0e38


def up(block):
    return block.astype(F32).reshape(block.shape[0] * 8, 128)


def tiles(rows):
    return rows.reshape(rows.shape[0] // 8, 8, 128).astype(BF16)


def iota(shape, dim):
    return lax.broadcasted_iota(jnp.int32, shape, dim)


def column_to_row(col):
    shape = (ROWS, 128)
    spread = jnp.where(iota(shape, 0) == iota(shape, 1), jnp.broadcast_to(col, shape), 0.0)
    return jnp.sum(spread, axis=0, keepdims=True)


def row_to_column(row):
    shape = (ROWS, 128)
    spread = jnp.where(iota(shape, 0) == iota(shape, 1), jnp.broadcast_to(row, shape), 0.0)
    return jnp.sum(spread, axis=1, keepdims=True)


def split_two(row):
    high = row.astype(BF16).astype(F32)
    return high, row - high


def with_rows(block, first, second):
    at = iota((ROWS, 128), 0)
    return jnp.where(at == SEQS, first, jnp.where(at == SEQS + 1, second, block))


def kernel(
    tok_hbm, again_hbm, wq_hbm, wk_hbm, wv_hbm, keys_hbm, vals_hbm, lam_hbm, hgain_hbm,
    wo_hbm, mgain_hbm, wg_hbm, wu_hbm, wd_hbm,
    out_ref,
    tok_v, again, wq, wk, wv, keys, vals, lam, hgain, wo, mgain, wg, wu, wd,
    x_all, x_rows,
    b_q, r_q, b_kv, r_kv, q_all, q_s, sc, o_s,
    b_o, r_o, m_s, l_s, h_all, r_b, res_t, b_g, r_g, hid, b_d, r_d,
    load_sem, send_sem, recv_sem,
):
    kv = lax.axis_index("kv")
    tp = lax.axis_index("tp")
    z = kv // N_X
    x = kv % N_X
    core = tp % 2

    def kv_peer(i):
        return ((z + i // N_X) % (N_KV // N_X)) * N_X + (x + i % N_X) % N_X

    def tp_peer(i):
        return (tp + i) % N_TP

    barrier = pltpu.get_barrier_semaphore()
    for i in range(1, N_TP):
        pl.semaphore_signal(barrier, inc=1, device_id=(kv, tp_peer(i)), device_id_type=MESH)
    for i in range(1, N_KV):
        pl.semaphore_signal(barrier, inc=1, device_id=(kv_peer(i), tp), device_id_type=MESH)

    loads = [
        pltpu.make_async_copy(src, dst, load_sem.at[n])
        for n, (src, dst) in enumerate(
            (
                (tok_hbm, tok_v), (again_hbm, again), (wq_hbm, wq), (wk_hbm, wk), (wv_hbm, wv),
                (keys_hbm, keys), (vals_hbm, vals), (lam_hbm, lam), (hgain_hbm, hgain),
                (wo_hbm, wo), (mgain_hbm, mgain), (wg_hbm, wg), (wu_hbm, wu),
                (wd_hbm, wd.at[pl.ds(0, wd_hbm.shape[0])]),
            )
        )
    ]
    for load in loads:
        load.start()
    (ld_tok, ld_again, ld_wq, ld_wk, ld_wv, ld_keys, ld_vals, ld_lam, ld_hgain, ld_wo, ld_mgain,
     ld_wg, ld_wu, ld_wd) = loads

    def copy_to(src, dst, phase, device):
        return pltpu.make_async_remote_copy(
            src_ref=src, dst_ref=dst, send_sem=send_sem.at[phase], recv_sem=recv_sem.at[phase],
            device_id=device, device_id_type=MESH,
        )

    def wait_bytes(ref, sem):
        pltpu.make_async_copy(ref, ref, sem).wait()

    wd[pl.ds(wd_hbm.shape[0], CHUNKS * 128 - wd_hbm.shape[0]), :] = jnp.zeros(
        (CHUNKS * 128 - wd_hbm.shape[0], 128), BF16
    )
    b_g[...] = jnp.zeros(b_g.shape, BF16)
    o_s[...] = jnp.zeros(o_s.shape, F32)
    for c in range(8):
        for s in range(SEQS, ROWS):
            sc[c, pl.ds(s, 8, stride=ROWS), :] = jnp.zeros((8, 128), F32)

    ld_tok.wait()
    x_all[tp] = jnp.concatenate(
        [tok_v[...].astype(F32), jnp.zeros((16, 128 - SEQS), F32)], axis=1
    ).astype(BF16)
    pl.semaphore_wait(barrier, N_TP - 1 + N_KV - 1)

    for i in range(1, N_TP):
        copy_to(x_all.at[tp], x_all.at[tp], 0, (kv, tp_peer(i))).start()
    ld_again.wait()
    ld_wq.wait()
    wait_bytes(x_all.at[pl.ds(0, N_TP - 1)], recv_sem.at[0])
    x_cols = x_all[...].astype(F32).reshape(128, 128)
    x_f = jnp.transpose(x_cols)[:ROWS]
    x_rows[...] = x_f
    normed = (x_f * again[...]).astype(BF16)
    square_row = column_to_row(jnp.sum(x_f * x_f, axis=1, keepdims=True))
    sq_high, sq_low = split_two(square_row)

    def head_owner(h):
        return 8 * h + 6 * core

    k_own = kv - 6 * core
    own_head = jnp.clip(k_own // 8, 0, HEADS - 1)
    is_head_owner = (kv == head_owner(own_head))

    q_part = jnp.dot(normed, wq[...], preferred_element_type=F32)
    for h in range(HEADS):
        b_q[h] = tiles(with_rows(q_part[:, h * 128 : (h + 1) * 128], sq_high, sq_low))
    for h in range(HEADS):
        owner = head_owner(h)
        slot = (kv - owner + N_KV) % N_KV

        @pl.when(owner != kv)
        def _():
            copy_to(b_q.at[h], r_q.at[slot], 1, (owner, tp)).start()

    ld_wk.wait()
    ld_wv.wait()
    k_part = jnp.dot(normed, wk[...], preferred_element_type=F32)
    v_part = jnp.dot(normed, wv[...], preferred_element_type=F32)
    for h in range(HEADS):
        b_kv[h, 0:3] = tiles(k_part[:, h * 128 : (h + 1) * 128])
        b_kv[h, 3:6] = tiles(v_part[:, h * 128 : (h + 1) * 128])
    for h in range(HEADS):
        owner = head_owner(h)
        slot = (kv - owner + N_KV) % N_KV

        @pl.when(owner != kv)
        def _():
            copy_to(b_kv.at[h], r_kv.at[slot], 2, (owner, tp)).start()

    @pl.when(is_head_owner)
    def _():
        wait_bytes(r_q.at[pl.ds(1, N_KV - 1)], recv_sem.at[1])
        total = up(b_q[own_head])
        for i in range(1, N_KV):
            total = total + up(r_q[i])
        square = total[SEQS : SEQS + 1] + total[SEQS + 1 : SEQS + 2]
        scale = row_to_column(lax.rsqrt(square / D + EPS))
        m_s[0, 0] = jnp.broadcast_to(scale, (ROWS, 128))
        q_all[own_head] = tiles(scale * total)
        for i in range(1, N_KV):
            copy_to(q_all.at[own_head], q_all.at[own_head], 3, (kv_peer(i), tp)).start()
        wait_bytes(q_all.at[pl.ds(0, HEADS - 1)], recv_sem.at[3])

    @pl.when(jnp.logical_not(is_head_owner))
    def _():
        wait_bytes(q_all, recv_sem.at[3])

    lane = iota((ROWS, 128), 1)
    for h in range(HEADS):
        q_h = up(q_all[h]) * 0.125
        q_s[pl.ds((2 * h) * ROWS, ROWS), :] = jnp.where(lane < 64, q_h, 0.0)
        q_s[pl.ds((2 * h + 1) * ROWS, ROWS), :] = jnp.where(lane >= 64, q_h, 0.0)
    ld_keys.wait()
    for s in range(SEQS):
        q_8 = q_s[pl.ds(s, 8, stride=ROWS), :].astype(BF16)
        part = lax.dot_general(
            q_8, keys[s], (((1,), (1,)), ((), ())), preferred_element_type=F32
        )
        for c in range(8):
            sc[c, pl.ds(s, 8, stride=ROWS), :] = part[:, c * 128 : (c + 1) * 128]

    for b in range(2 * HEADS):
        rows = pl.ds(b * ROWS, ROWS)
        mine = (iota((ROWS, 128), 1) % HEADS) == (b // 2)
        top = sc[0, rows, :]
        for c in range(1, 8):
            top = jnp.maximum(top, sc[c, rows, :])
        top = jnp.max(jnp.where(mine, top, LOW), axis=1, keepdims=True)
        total = jnp.zeros((ROWS, 128), F32)
        for c in range(8):
            weight = jnp.where(mine, jnp.exp(jnp.where(mine, sc[c, rows, :], LOW) - top), 0.0)
            sc[c, rows, :] = weight
            total = total + weight
        total = jnp.sum(total, axis=1, keepdims=True)
        m_s[1 + b // 2, b % 2] = jnp.broadcast_to(top, (ROWS, 128))
        l_s[1 + b // 2, b % 2] = jnp.broadcast_to(total, (ROWS, 128))

    ld_vals.wait()
    for s in range(SEQS):
        w_8 = jnp.concatenate(
            [sc[c, pl.ds(s, 8, stride=ROWS), :] for c in range(8)], axis=1
        ).astype(BF16)
        o_s[pl.ds(s, 8, stride=ROWS), :] = jnp.dot(w_8, vals[s], preferred_element_type=F32)

    def stat_row(col_b):
        shape = (ROWS, 128)
        row = jnp.sum(jnp.where(iota(shape, 0) == iota(shape, 1), col_b, 0.0), axis=0, keepdims=True)
        high = row.astype(BF16).astype(F32)
        mid = (row - high).astype(BF16).astype(F32)
        low = (row - high - mid).astype(BF16).astype(F32)
        at = iota((8, 128), 1)
        high, mid, low = (jnp.broadcast_to(v, (8, 128)) for v in (high, mid, low))
        packed = jnp.where(
            at < 32, high, jnp.where(at < 64, pltpu.roll(mid, 32, 1), pltpu.roll(low, 64, 1))
        )
        return packed[0:1]

    for b in range(2 * HEADS):
        h, mp = b // 2, b % 2
        block = with_rows(
            o_s[pl.ds(b * ROWS, ROWS), :], stat_row(m_s[1 + h, mp]), stat_row(l_s[1 + h, mp])
        )
        b_o[h, 3 * mp : 3 * mp + 3] = tiles(block)
    for h in range(HEADS):
        owner = head_owner(h)
        slot = (kv - owner + N_KV) % N_KV

        @pl.when(owner != kv)
        def _():
            copy_to(b_o.at[h], r_o.at[slot], 4, (owner, tp)).start()

    @pl.when(is_head_owner)
    def _():
        scale = m_s[0, 0]
        wait_bytes(r_kv.at[pl.ds(1, N_KV - 1)], recv_sem.at[2])
        k_sum = up(b_kv[own_head, 0:3])
        v_sum = up(b_kv[own_head, 3:6])
        for i in range(1, N_KV):
            k_sum = k_sum + up(r_kv[i, 0:3])
            v_sum = v_sum + up(r_kv[i, 3:6])
        k_new = (scale * k_sum).astype(BF16).astype(F32)
        v_new = (scale * v_sum).astype(BF16).astype(F32)
        product = up(q_all[own_head]) * k_new
        wait_bytes(r_o.at[pl.ds(1, N_KV - 1)], recv_sem.at[4])
        r_o[0] = b_o[own_head]
        pieces = iota((ROWS, 128), 1) % 32 == iota((ROWS, 128), 0)
        pieces = jnp.logical_and(pieces, iota((ROWS, 128), 1) < 96)

        def stat_col(row):
            spread = jnp.where(pieces, jnp.broadcast_to(row, (ROWS, 128)), 0.0)
            return jnp.broadcast_to(jnp.sum(spread, axis=1, keepdims=True), (ROWS, 128))

        results = []
        for mp in range(2):
            half = jnp.where((lane < 64) == (mp == 0), product, 0.0)
            new = jnp.sum(half, axis=1, keepdims=True) * 0.125
            peak = jnp.broadcast_to(new, (ROWS, 128))
            for i in range(N_KV):
                tile = r_o[i, 3 * mp + 2].astype(F32)
                m_i = stat_col(tile[6:7])
                l_s[i, mp] = stat_col(tile[7:8])
                m_s[i, mp] = m_i
                peak = jnp.maximum(peak, m_i)
            weight = jnp.exp(jnp.broadcast_to(new, (ROWS, 128)) - peak)
            numer = weight * v_new
            denom = weight
            for i in range(N_KV):
                weight = jnp.exp(m_s[i, mp] - peak)
                numer = numer + weight * up(r_o[i, 3 * mp : 3 * mp + 3])
                denom = denom + weight * l_s[i, mp]
            results.append(numer / denom)
        ld_lam.wait()
        ld_hgain.wait()
        mine = iota((1, HEADS), 1) == own_head
        lam_h = jnp.sum(jnp.where(mine, lam[...], 0.0), axis=1, keepdims=True)
        difference = results[0] - lam_h * results[1]
        mean = jnp.mean(difference * difference, axis=1, keepdims=True)
        h_all[own_head] = tiles(difference * lax.rsqrt(mean + EPS) * hgain[...])
        for i in range(1, N_KV):
            copy_to(h_all.at[own_head], h_all.at[own_head], 5, (kv_peer(i), tp)).start()
        wait_bytes(h_all.at[pl.ds(0, HEADS - 1)], recv_sem.at[5])

    @pl.when(jnp.logical_not(is_head_owner))
    def _():
        ld_lam.wait()
        ld_hgain.wait()
        wait_bytes(h_all, recv_sem.at[5])

    ld_wo.wait()
    heads_out = jnp.concatenate([up(h_all[h]) for h in range(HEADS)], axis=1).astype(BF16)
    r_b[tp] = tiles(jnp.dot(heads_out, wo[...], preferred_element_type=F32))
    for i in range(1, N_TP):
        copy_to(r_b.at[tp], r_b.at[tp], 6, (kv, tp_peer(i))).start()
    ld_mgain.wait()
    ld_wg.wait()
    ld_wu.wait()
    wait_bytes(r_b.at[pl.ds(0, N_TP - 1)], recv_sem.at[6])
    branch = up(r_b[0])
    for i in range(1, N_TP):
        branch = branch + up(r_b[i])
    live = iota((ROWS, 128), 0) < SEQS
    residual = jnp.where(live, (x_rows[...] + branch).astype(BF16).astype(F32), 0.0)
    normed_mid = (residual * mgain[...]).astype(BF16)
    sq_high, sq_low = split_two(
        column_to_row(jnp.sum(residual * residual, axis=1, keepdims=True))
    )

    across = (((1,), (1,)), ((), ()))
    gate_part = lax.dot_general(normed_mid, wg[...], across, preferred_element_type=F32)
    up_part = lax.dot_general(normed_mid, wu[...], across, preferred_element_type=F32)
    width = gate_part.shape[1]
    for j in range(CHUNKS):
        lo, hi = j * 128, min(j * 128 + 128, width)
        n = hi - lo
        at = iota((ROWS, n), 0)
        g_j = jnp.where(
            at == SEQS, sq_high[:, :n], jnp.where(at == SEQS + 1, sq_low[:, :n], gate_part[:, lo:hi])
        )
        u_j = up_part[:, lo:hi]
        b_g[j, 0:3, :, 0:n] = g_j.reshape(3, 8, n).astype(BF16)
        b_g[j, 3:6, :, 0:n] = u_j.reshape(3, 8, n).astype(BF16)

    def chunk_owner(j):
        return (32 * j) // CHUNKS + core

    k_chunk = kv - core
    own_chunk = jnp.clip((CHUNKS * k_chunk + 31) // 32, 0, CHUNKS - 1)
    is_chunk_owner = chunk_owner(own_chunk) == kv
    for j in range(CHUNKS):
        owner = chunk_owner(j)
        slot = (kv - owner + N_KV) % N_KV

        @pl.when(owner != kv)
        def _():
            copy_to(b_g.at[j], r_g.at[slot], 7, (owner, tp)).start()

    res_t[...] = jnp.transpose(
        jnp.concatenate([residual, jnp.zeros((128 - ROWS, 128), F32)], axis=0)
    ).reshape(N_TP, 16, 128)

    @pl.when(is_chunk_owner)
    def _():
        wait_bytes(r_g.at[pl.ds(1, N_KV - 1)], recv_sem.at[7])
        gate = up(b_g[own_chunk, 0:3])
        upper = up(b_g[own_chunk, 3:6])
        for i in range(1, N_KV):
            gate = gate + up(r_g[i, 0:3])
            upper = upper + up(r_g[i, 3:6])
        square = gate[SEQS : SEQS + 1] + gate[SEQS + 1 : SEQS + 2]
        scale = row_to_column(lax.rsqrt(square / D + EPS))
        gate = scale * gate
        hidden = (gate / (1.0 + jnp.exp(-gate))) * (scale * upper)
        hid[own_chunk] = tiles(hidden)
        for i in range(1, N_KV):
            copy_to(hid.at[own_chunk], hid.at[own_chunk], 8, (kv_peer(i), tp)).start()
        wait_bytes(hid.at[pl.ds(0, CHUNKS - 1)], recv_sem.at[8])

    @pl.when(jnp.logical_not(is_chunk_owner))
    def _():
        wait_bytes(hid, recv_sem.at[8])

    ld_wd.wait()
    hidden_all = jnp.concatenate([up(hid[j]) for j in range(CHUNKS)], axis=1).astype(BF16)
    down = jnp.dot(hidden_all, wd[...], preferred_element_type=F32)
    down_t = jnp.transpose(
        jnp.concatenate([down, jnp.zeros((128 - ROWS, 128), F32)], axis=0)
    )
    b_d[...] = down_t.reshape(N_TP, 16, 128).astype(BF16)
    r_d[tp] = b_d[tp]
    for i in range(1, N_TP):
        peer = tp_peer(i)
        copy_to(b_d.at[peer], r_d.at[tp], 9, (kv, peer)).start()
    wait_bytes(r_d.at[pl.ds(0, N_TP - 1)], recv_sem.at[9])
    mixer = r_d[0].astype(F32)
    for i in range(1, N_TP):
        mixer = mixer + r_d[i].astype(F32)
    out_ref[...] = (res_t[tp] + mixer).astype(BF16)[:, :SEQS]

    wait_bytes(x_all.at[pl.ds(0, N_TP - 1)], send_sem.at[0])
    wait_bytes(r_b.at[pl.ds(0, N_TP - 1)], send_sem.at[6])
    wait_bytes(r_d.at[pl.ds(0, N_TP - 1)], send_sem.at[9])

    @pl.when(is_head_owner)
    def _():
        wait_bytes(r_q.at[pl.ds(0, HEADS - 1)], send_sem.at[1])
        wait_bytes(r_kv.at[pl.ds(0, HEADS - 1)], send_sem.at[2])
        wait_bytes(r_q.at[pl.ds(1, N_KV - 1)], send_sem.at[3])
        wait_bytes(r_o.at[pl.ds(0, HEADS - 1)], send_sem.at[4])
        wait_bytes(r_q.at[pl.ds(1, N_KV - 1)], send_sem.at[5])

    @pl.when(jnp.logical_not(is_head_owner))
    def _():
        wait_bytes(r_q.at[pl.ds(0, HEADS)], send_sem.at[1])
        wait_bytes(r_kv.at[pl.ds(0, HEADS)], send_sem.at[2])
        wait_bytes(r_o.at[pl.ds(0, HEADS)], send_sem.at[4])

    @pl.when(is_chunk_owner)
    def _():
        wait_bytes(r_g.at[pl.ds(0, CHUNKS - 1)], send_sem.at[7])
        wait_bytes(r_q.at[pl.ds(1, N_KV - 1)], send_sem.at[8])

    @pl.when(jnp.logical_not(is_chunk_owner))
    def _():
        wait_bytes(r_g.at[pl.ds(0, CHUNKS)], send_sem.at[7])


def per_device(
    tokens, attn_gain, w_query, w_key, w_value, cache_keys, cache_values, lambdas, head_gain,
    w_out, mlp_gain, w_gate, w_up, w_down,
):
    seqs, positions, heads, dim = cache_keys.shape
    args = (
        tokens.T, attn_gain.reshape(1, -1), w_query, w_key, w_value,
        cache_keys.reshape(seqs, positions * heads, dim),
        cache_values.reshape(seqs, positions * heads, dim),
        lambdas.reshape(1, -1), head_gain.reshape(1, -1), w_out, mlp_gain.reshape(1, -1),
        w_gate.T, w_up.T, w_down,
    )
    vmem = pltpu.VMEM
    local = [vmem(a.shape, a.dtype) for a in args]
    local[-1] = vmem((CHUNKS * 128, 128), BF16)
    tile = (3, 8, 128)
    pair = (6, 8, 128)
    scratch = local + [
        vmem((N_TP, 16, 128), BF16),
        vmem((ROWS, 128), F32),
        vmem((HEADS, *tile), BF16),
        vmem((N_KV, *tile), BF16),
        vmem((HEADS, *pair), BF16),
        vmem((N_KV, *pair), BF16),
        vmem((HEADS, *tile), BF16),
        vmem((2 * HEADS * ROWS, 128), F32),
        vmem((8, 2 * HEADS * ROWS, 128), F32),
        vmem((2 * HEADS * ROWS, 128), F32),
        vmem((HEADS, *pair), BF16),
        vmem((N_KV, *pair), BF16),
        vmem((N_KV, 2, ROWS, 128), F32),
        vmem((N_KV, 2, ROWS, 128), F32),
        vmem((HEADS, *tile), BF16),
        vmem((N_TP, *tile), BF16),
        vmem((N_TP, 16, 128), F32),
        vmem((CHUNKS, *pair), BF16),
        vmem((N_KV, *pair), BF16),
        vmem((CHUNKS, *tile), BF16),
        vmem((N_TP, 16, 128), BF16),
        vmem((N_TP, 16, 128), BF16),
        pltpu.SemaphoreType.DMA((len(args),)),
        pltpu.SemaphoreType.DMA((10,)),
        pltpu.SemaphoreType.DMA((10,)),
    ]
    out = pl.pallas_call(
        kernel,
        out_shape=jax.ShapeDtypeStruct((tokens.shape[1], seqs), BF16),
        in_specs=[pl.BlockSpec(memory_space=pl.ANY)] * len(args),
        out_specs=pl.BlockSpec(memory_space=pltpu.VMEM),
        scratch_shapes=scratch,
        compiler_params=pltpu.CompilerParams(
            collective_id=0, has_side_effects=True, vmem_limit_bytes=60 * 1024 * 1024
        ),
        name="decode_step",
    )(*args)
    return out.T


def solution(mesh):
    placed = (
        P(None, ("kv", "tp")), P("kv"), P("kv", "tp"), P("kv", "tp"), P("kv", "tp"),
        P(None, "kv", "tp", None), P(None, "kv", "tp", None), P("tp"), P(), P("tp", "kv"),
        P("kv"), P("kv", "tp"), P("kv", "tp"), P("tp", "kv"),
    )
    return jax.shard_map(
        per_device, mesh=mesh, in_specs=placed, out_specs=P(None, ("kv", "tp")), check_vma=False
    )
```

```python
import functools

import jax
import jax.numpy as jnp
from jax import lax
from jax.experimental import pallas as pl
from jax.experimental.pallas import tpu as pltpu
from jax.sharding import PartitionSpec as P

MESH = pl.DeviceIdType.MESH
F32, BF16 = jnp.float32, jnp.bfloat16
D = 4096
EPS = 1e-06
ROWS = 24
SEQS = 22
N_KV, N_X, N_TP = 32, 4, 8
N_Z = N_KV // N_X
KV_ORDER = sorted(
    range(1, N_KV),
    key=lambda i: -(min(i // N_X, N_Z - i // N_X) + min(i % N_X, N_X - i % N_X)),
)
TP_ORDER = (4, 5, 3, 2, 6, 7, 1)
PLANES = sorted(range(N_Z), key=lambda p: min(p, N_Z - p))
HEADS = 4
CHUNKS = 11
LOW = -3.0e38
QUERY_OWNERS = ((0, 8, 16, 24), (6, 14, 22, 30))
HEAD_OWNERS = ((0, 6, 8, 14), (1, 7, 9, 15))
CHUNK_OWNERS = ((0, 2, 5, 8, 11, 14, 17, 20, 23, 26, 29), (1, 3, 6, 9, 12, 15, 18, 21, 24, 27, 30))


def up(block):
    return block.astype(F32).reshape(block.shape[0] * 8, 128)


def tiles(rows):
    return rows.reshape(rows.shape[0] // 8, 8, 128).astype(BF16)


def iota(shape, dim):
    return lax.broadcasted_iota(jnp.int32, shape, dim)


def column_to_row(col):
    shape = (ROWS, 128)
    spread = jnp.where(iota(shape, 0) == iota(shape, 1), jnp.broadcast_to(col, shape), 0.0)
    return jnp.sum(spread, axis=0, keepdims=True)


def row_to_column(row):
    shape = (ROWS, 128)
    spread = jnp.where(iota(shape, 0) == iota(shape, 1), jnp.broadcast_to(row, shape), 0.0)
    return jnp.sum(spread, axis=1, keepdims=True)


def split_two(row):
    high = row.astype(BF16).astype(F32)
    return high, row - high


def with_rows(block, first, second):
    at = iota((ROWS, 128), 0)
    return jnp.where(at == SEQS, first, jnp.where(at == SEQS + 1, second, block))


def kernel(
    tok_hbm, again_hbm, wq_hbm, wk_hbm, wv_hbm, keys_hbm, vals_hbm, lam_hbm, hgain_hbm,
    wo_hbm, mgain_hbm, wg_hbm, wu_hbm, wd_hbm,
    out_ref,
    tok_v, again, wq, wk, wv, keys, vals, lam, hgain, wo, mgain, wg, wu, wd,
    x_all, x_rows,
    b_q, r_q, b_kv, r_kv, q_all, q_s, sc, o_s,
    b_o, r_o, m_s, l_s, h_all, r_b, res_t, b_g, r_g, hid, b_d, r_d,
    keys_t, load_sem, send_sem, recv_sem,
):
    kv = lax.axis_index("kv")
    tp = lax.axis_index("tp")
    z = kv // N_X
    x = kv % N_X
    core = tp % 2

    def kv_slot(owner):
        return ((z - owner // N_X) % N_Z) * N_X + (x - owner % N_X) % N_X

    def kv_peer(i):
        return ((z + i // N_X) % N_Z) * N_X + (x + i % N_X) % N_X

    def tp_peer(i):
        return (tp + i) % N_TP

    def owner_in(table, n):
        return table[0][n] + (table[1][n] - table[0][n]) * core

    def own_in(table):
        at = [(kv == owner_in(table, n)).astype(jnp.int32) for n in range(len(table[0]))]
        return sum(n * hit for n, hit in enumerate(at)), sum(at) > 0

    query_head, is_query_owner = own_in(QUERY_OWNERS)
    own_head, is_head_owner = own_in(HEAD_OWNERS)
    own_chunk, is_chunk_owner = own_in(CHUNK_OWNERS)

    barrier = pltpu.get_barrier_semaphore()
    for i in range(1, N_TP):
        pl.semaphore_signal(barrier, inc=1, device_id=(kv, tp_peer(i)), device_id_type=MESH)

    for role in (is_query_owner, is_head_owner):

        @pl.when(role)
        def _():
            for i in KV_ORDER:
                pl.semaphore_signal(barrier, inc=1, device_id=(kv_peer(i), tp), device_id_type=MESH)

    loads = [
        pltpu.make_async_copy(src, dst, load_sem.at[n])
        for n, (src, dst) in enumerate(
            (
                (tok_hbm, tok_v), (again_hbm, again), (wq_hbm, wq), (wk_hbm, wk), (wv_hbm, wv),
                (keys_hbm, keys), (vals_hbm, vals), (lam_hbm, lam), (hgain_hbm, hgain),
                (wo_hbm, wo), (mgain_hbm, mgain), (wg_hbm, wg), (wu_hbm, wu),
                (wd_hbm, wd.at[pl.ds(0, wd_hbm.shape[0])]),
            )
        )
    ]
    for load in loads:
        load.start()
    (ld_tok, ld_again, ld_wq, ld_wk, ld_wv, ld_keys, ld_vals, ld_lam, ld_hgain, ld_wo, ld_mgain,
     ld_wg, ld_wu, ld_wd) = loads

    def copy_to(src, dst, phase, device, plane=0):
        return pltpu.make_async_remote_copy(
            src_ref=src, dst_ref=dst, send_sem=send_sem.at[phase],
            recv_sem=recv_sem.at[phase, plane], device_id=device, device_id_type=MESH,
        )

    def plane_slots(ref, phase, p):
        first = 1 if p == 0 else p * N_X
        count = p * N_X + N_X - first
        wait_bytes(ref.at[pl.ds(first, count)], recv_sem.at[phase, p])
        return range(first, first + count)

    def wait_bytes(ref, sem):
        pltpu.make_async_copy(ref, ref, sem).wait()

    wd[pl.ds(wd_hbm.shape[0], CHUNKS * 128 - wd_hbm.shape[0]), :] = jnp.zeros(
        (CHUNKS * 128 - wd_hbm.shape[0], 128), BF16
    )
    b_g[...] = jnp.zeros(b_g.shape, BF16)
    o_s[...] = jnp.zeros(o_s.shape, F32)
    for c in range(8):
        for s in range(SEQS, ROWS):
            sc[c, pl.ds(s, 8, stride=ROWS), :] = jnp.zeros((8, 128), F32)

    ld_tok.wait()
    x_all[tp] = jnp.concatenate(
        [tok_v[...].astype(F32), jnp.zeros((16, 128 - SEQS), F32)], axis=1
    ).astype(BF16)
    own_roles = is_query_owner.astype(jnp.int32) + is_head_owner.astype(jnp.int32)
    pl.semaphore_wait(barrier, N_TP - 1 + 2 * HEADS - own_roles)

    for i in TP_ORDER:
        copy_to(x_all.at[tp], x_all.at[tp], 0, (kv, tp_peer(i))).start()
    ld_again.wait()
    ld_wq.wait()
    wait_bytes(x_all.at[pl.ds(0, N_TP - 1)], recv_sem.at[0, 0])
    x_cols = x_all[...].astype(F32).reshape(128, 128)
    x_f = jnp.transpose(x_cols)[:ROWS]
    x_rows[...] = x_f
    normed = (x_f * again[...]).astype(BF16)
    square_row = column_to_row(jnp.sum(x_f * x_f, axis=1, keepdims=True))
    sq_high, sq_low = split_two(square_row)

    q_part = jnp.dot(normed, wq[...], preferred_element_type=F32)
    for h in range(HEADS):
        b_q[h] = tiles(with_rows(q_part[:, h * 128 : (h + 1) * 128], sq_high, sq_low))
    for h in range(HEADS):
        owner = owner_in(QUERY_OWNERS, h)
        slot = kv_slot(owner)

        @pl.when(owner != kv)
        def _():
            copy_to(b_q.at[h], r_q.at[slot], 1, (owner, tp), slot // N_X).start()

    ld_wk.wait()
    ld_wv.wait()
    k_part = jnp.dot(normed, wk[...], preferred_element_type=F32)
    v_part = jnp.dot(normed, wv[...], preferred_element_type=F32)
    for h in range(HEADS):
        b_kv[h, 0:3] = tiles(with_rows(k_part[:, h * 128 : (h + 1) * 128], sq_high, sq_low))
        b_kv[h, 3:6] = tiles(v_part[:, h * 128 : (h + 1) * 128])
    for h in range(HEADS):
        owner = owner_in(HEAD_OWNERS, h)
        slot = kv_slot(owner)

        @pl.when(owner != kv)
        def _():
            copy_to(b_kv.at[h], r_kv.at[slot], 2, (owner, tp), slot // N_X).start()

    @pl.when(is_query_owner)
    def _():
        total = up(b_q[query_head])
        for p in PLANES:
            for i in plane_slots(r_q, 1, p):
                total = total + up(r_q[i])
        square = total[SEQS : SEQS + 1] + total[SEQS + 1 : SEQS + 2]
        scale = row_to_column(lax.rsqrt(square / D + EPS))
        q_all[query_head] = tiles(scale * total)
        for i in KV_ORDER:
            copy_to(q_all.at[query_head], q_all.at[query_head], 3, (kv_peer(i), tp)).start()

    ld_keys.wait()
    for s in range(SEQS):
        keys_t[s] = jnp.transpose(keys[s])

    role = is_query_owner

    @pl.when(role)
    def _():
        wait_bytes(q_all.at[pl.ds(0, HEADS - 1)], recv_sem.at[3, 0])

    @pl.when(jnp.logical_not(role))
    def _():
        wait_bytes(q_all, recv_sem.at[3, 0])

    lane = iota((ROWS, 128), 1)
    for h in range(HEADS):
        q_h = up(q_all[h]) * 0.125
        q_s[pl.ds((2 * h) * ROWS, ROWS), :] = jnp.where(lane < 64, q_h, 0.0)
        q_s[pl.ds((2 * h + 1) * ROWS, ROWS), :] = jnp.where(lane >= 64, q_h, 0.0)
    for s in range(SEQS):
        q_8 = q_s[pl.ds(s, 8, stride=ROWS), :].astype(BF16)
        part = jnp.dot(q_8, keys_t[s], preferred_element_type=F32)
        for c in range(8):
            sc[c, pl.ds(s, 8, stride=ROWS), :] = part[:, c * 128 : (c + 1) * 128]

    for b in range(2 * HEADS):
        rows = pl.ds(b * ROWS, ROWS)
        mine = (iota((ROWS, 128), 1) % HEADS) == (b // 2)
        top = sc[0, rows, :]
        for c in range(1, 8):
            top = jnp.maximum(top, sc[c, rows, :])
        top = jnp.max(jnp.where(mine, top, LOW), axis=1, keepdims=True)
        total = jnp.zeros((ROWS, 128), F32)
        for c in range(8):
            weight = jnp.where(mine, jnp.exp(jnp.where(mine, sc[c, rows, :], LOW) - top), 0.0)
            sc[c, rows, :] = weight
            total = total + weight
        total = jnp.sum(total, axis=1, keepdims=True)
        m_s[1 + b // 2, b % 2] = jnp.broadcast_to(top, (ROWS, 128))
        l_s[1 + b // 2, b % 2] = jnp.broadcast_to(total, (ROWS, 128))

    ld_vals.wait()
    for s in range(SEQS):
        w_8 = jnp.concatenate(
            [sc[c, pl.ds(s, 8, stride=ROWS), :] for c in range(8)], axis=1
        ).astype(BF16)
        o_s[pl.ds(s, 8, stride=ROWS), :] = jnp.dot(w_8, vals[s], preferred_element_type=F32)

    def stat_row(col_b):
        shape = (ROWS, 128)
        row = jnp.sum(jnp.where(iota(shape, 0) == iota(shape, 1), col_b, 0.0), axis=0, keepdims=True)
        high = row.astype(BF16).astype(F32)
        mid = (row - high).astype(BF16).astype(F32)
        low = (row - high - mid).astype(BF16).astype(F32)
        at = iota((8, 128), 1)
        high, mid, low = (jnp.broadcast_to(v, (8, 128)) for v in (high, mid, low))
        packed = jnp.where(
            at < 32, high, jnp.where(at < 64, pltpu.roll(mid, 32, 1), pltpu.roll(low, 64, 1))
        )
        return packed[0:1]

    for b in range(2 * HEADS):
        h, mp = b // 2, b % 2
        block = with_rows(
            o_s[pl.ds(b * ROWS, ROWS), :], stat_row(m_s[1 + h, mp]), stat_row(l_s[1 + h, mp])
        )
        b_o[h, 3 * mp : 3 * mp + 3] = tiles(block)
    for h in range(HEADS):
        owner = owner_in(HEAD_OWNERS, h)
        slot = kv_slot(owner)

        @pl.when(owner != kv)
        def _():
            copy_to(b_o.at[h], r_o.at[slot], 4, (owner, tp), slot // N_X).start()

    @pl.when(is_head_owner)
    def _():
        k_sum = up(b_kv[own_head, 0:3])
        v_sum = up(b_kv[own_head, 3:6])
        for p in PLANES:
            for i in plane_slots(r_kv, 2, p):
                k_sum = k_sum + up(r_kv[i, 0:3])
                v_sum = v_sum + up(r_kv[i, 3:6])
        square = k_sum[SEQS : SEQS + 1] + k_sum[SEQS + 1 : SEQS + 2]
        scale = row_to_column(lax.rsqrt(square / D + EPS))
        k_new = (scale * k_sum).astype(BF16).astype(F32)
        v_new = (scale * v_sum).astype(BF16).astype(F32)
        product = up(q_all[own_head]) * k_new
        r_o[0] = b_o[own_head]
        pieces = iota((ROWS, 128), 1) % 32 == iota((ROWS, 128), 0)
        pieces = jnp.logical_and(pieces, iota((ROWS, 128), 1) < 96)

        def stat_col(row):
            spread = jnp.where(pieces, jnp.broadcast_to(row, (ROWS, 128)), 0.0)
            return jnp.broadcast_to(jnp.sum(spread, axis=1, keepdims=True), (ROWS, 128))

        peak, denom, numer = [], [], []
        for mp in range(2):
            half = jnp.where((lane < 64) == (mp == 0), product, 0.0)
            new = jnp.sum(half, axis=1, keepdims=True) * 0.125
            peak.append(jnp.broadcast_to(new, (ROWS, 128)))
            denom.append(jnp.ones((ROWS, 128), F32))
            numer.append(v_new)
        for p in PLANES:
            slots = list(plane_slots(r_o, 4, p))
            if p == 0:
                slots.append(0)
            for mp in range(2):
                last = [r_o[i, 3 * mp + 2].astype(F32) for i in slots]
                tops = [stat_col(tile[6:7]) for tile in last]
                totals = [stat_col(tile[7:8]) for tile in last]
                above = functools.reduce(jnp.maximum, tops, peak[mp])
                fade = jnp.exp(peak[mp] - above)
                n, d = numer[mp] * fade, denom[mp] * fade
                for i, top, total in zip(slots, tops, totals):
                    weight = jnp.exp(top - above)
                    n = n + weight * up(r_o[i, 3 * mp : 3 * mp + 3])
                    d = d + weight * total
                peak[mp], numer[mp], denom[mp] = above, n, d
        results = [numer[mp] / denom[mp] for mp in range(2)]
        ld_lam.wait()
        ld_hgain.wait()
        mine = iota((1, HEADS), 1) == own_head
        lam_h = jnp.sum(jnp.where(mine, lam[...], 0.0), axis=1, keepdims=True)
        difference = results[0] - lam_h * results[1]
        mean = jnp.mean(difference * difference, axis=1, keepdims=True)
        h_all[own_head] = tiles(difference * lax.rsqrt(mean + EPS) * hgain[...])
        for i in KV_ORDER:
            copy_to(h_all.at[own_head], h_all.at[own_head], 5, (kv_peer(i), tp)).start()
        wait_bytes(h_all.at[pl.ds(0, HEADS - 1)], recv_sem.at[5, 0])

    @pl.when(jnp.logical_not(is_head_owner))
    def _():
        ld_lam.wait()
        ld_hgain.wait()
        wait_bytes(h_all, recv_sem.at[5, 0])

    ld_wo.wait()
    heads_out = jnp.concatenate([up(h_all[h]) for h in range(HEADS)], axis=1).astype(BF16)
    r_b[tp] = tiles(jnp.dot(heads_out, wo[...], preferred_element_type=F32))
    for i in TP_ORDER:
        copy_to(r_b.at[tp], r_b.at[tp], 6, (kv, tp_peer(i))).start()
    ld_mgain.wait()
    ld_wg.wait()
    ld_wu.wait()
    wait_bytes(r_b.at[pl.ds(0, N_TP - 1)], recv_sem.at[6, 0])
    branch = up(r_b[0])
    for i in range(1, N_TP):
        branch = branch + up(r_b[i])
    live = iota((ROWS, 128), 0) < SEQS
    residual = jnp.where(live, (x_rows[...] + branch).astype(BF16).astype(F32), 0.0)
    normed_mid = (residual * mgain[...]).astype(BF16)
    sq_high, sq_low = split_two(
        column_to_row(jnp.sum(residual * residual, axis=1, keepdims=True))
    )

    across = (((1,), (1,)), ((), ()))
    width = wg.shape[0]
    for j in range(CHUNKS):
        lo, hi = j * 128, min(j * 128 + 128, width)
        n = hi - lo
        at = iota((ROWS, n), 0)
        g_j = lax.dot_general(normed_mid, wg[lo:hi, :], across, preferred_element_type=F32)
        u_j = lax.dot_general(normed_mid, wu[lo:hi, :], across, preferred_element_type=F32)
        g_j = jnp.where(at == SEQS, sq_high[:, :n], jnp.where(at == SEQS + 1, sq_low[:, :n], g_j))
        b_g[j, 0:3, :, 0:n] = g_j.reshape(3, 8, n).astype(BF16)
        b_g[j, 3:6, :, 0:n] = u_j.reshape(3, 8, n).astype(BF16)
        owner = owner_in(CHUNK_OWNERS, j)
        slot = kv_slot(owner)

        @pl.when(owner != kv)
        def _():
            copy_to(b_g.at[j], r_g.at[slot], 7, (owner, tp), slot // N_X).start()

    res_t[...] = jnp.transpose(
        jnp.concatenate([residual, jnp.zeros((128 - ROWS, 128), F32)], axis=0)
    ).reshape(N_TP, 16, 128)

    @pl.when(is_chunk_owner)
    def _():
        gate = up(b_g[own_chunk, 0:3])
        upper = up(b_g[own_chunk, 3:6])
        for p in PLANES:
            for i in plane_slots(r_g, 7, p):
                gate = gate + up(r_g[i, 0:3])
                upper = upper + up(r_g[i, 3:6])
        square = gate[SEQS : SEQS + 1] + gate[SEQS + 1 : SEQS + 2]
        scale = row_to_column(lax.rsqrt(square / D + EPS))
        gate = scale * gate
        hidden = (gate / (1.0 + jnp.exp(-gate))) * (scale * upper)
        hid[own_chunk] = tiles(hidden)
        for i in KV_ORDER:
            copy_to(hid.at[own_chunk], hid.at[own_chunk], 8, (kv_peer(i), tp)).start()
        wait_bytes(hid.at[pl.ds(0, CHUNKS - 1)], recv_sem.at[8, 0])

    @pl.when(jnp.logical_not(is_chunk_owner))
    def _():
        wait_bytes(hid, recv_sem.at[8, 0])

    ld_wd.wait()
    hidden_all = jnp.concatenate([up(hid[j]) for j in range(CHUNKS)], axis=1).astype(BF16)
    down = jnp.dot(hidden_all, wd[...], preferred_element_type=F32)
    down_t = jnp.transpose(
        jnp.concatenate([down, jnp.zeros((128 - ROWS, 128), F32)], axis=0)
    )
    b_d[...] = down_t.reshape(N_TP, 16, 128).astype(BF16)
    r_d[tp] = b_d[tp]
    for i in TP_ORDER:
        peer = tp_peer(i)
        copy_to(b_d.at[peer], r_d.at[tp], 9, (kv, peer)).start()
    wait_bytes(r_d.at[pl.ds(0, N_TP - 1)], recv_sem.at[9, 0])
    mixer = r_d[0].astype(F32)
    for i in range(1, N_TP):
        mixer = mixer + r_d[i].astype(F32)
    out_ref[...] = (res_t[tp] + mixer).astype(BF16)[:, :SEQS]

    wait_bytes(x_all.at[pl.ds(0, N_TP - 1)], send_sem.at[0])
    wait_bytes(r_b.at[pl.ds(0, N_TP - 1)], send_sem.at[6])
    wait_bytes(r_d.at[pl.ds(0, N_TP - 1)], send_sem.at[9])

    @pl.when(is_query_owner)
    def _():
        wait_bytes(r_q.at[pl.ds(0, HEADS - 1)], send_sem.at[1])
        wait_bytes(r_q.at[pl.ds(1, N_KV - 1)], send_sem.at[3])

    @pl.when(jnp.logical_not(is_query_owner))
    def _():
        wait_bytes(r_q.at[pl.ds(0, HEADS)], send_sem.at[1])

    @pl.when(is_head_owner)
    def _():
        wait_bytes(r_kv.at[pl.ds(0, HEADS - 1)], send_sem.at[2])
        wait_bytes(r_o.at[pl.ds(0, HEADS - 1)], send_sem.at[4])
        wait_bytes(r_q.at[pl.ds(1, N_KV - 1)], send_sem.at[5])

    @pl.when(jnp.logical_not(is_head_owner))
    def _():
        wait_bytes(r_kv.at[pl.ds(0, HEADS)], send_sem.at[2])
        wait_bytes(r_o.at[pl.ds(0, HEADS)], send_sem.at[4])

    @pl.when(is_chunk_owner)
    def _():
        wait_bytes(r_g.at[pl.ds(0, CHUNKS - 1)], send_sem.at[7])
        wait_bytes(r_q.at[pl.ds(1, N_KV - 1)], send_sem.at[8])

    @pl.when(jnp.logical_not(is_chunk_owner))
    def _():
        wait_bytes(r_g.at[pl.ds(0, CHUNKS)], send_sem.at[7])


def per_device(
    tokens, attn_gain, w_query, w_key, w_value, cache_keys, cache_values, lambdas, head_gain,
    w_out, mlp_gain, w_gate, w_up, w_down,
):
    seqs, positions, heads, dim = cache_keys.shape
    args = (
        tokens.T, attn_gain.reshape(1, -1), w_query, w_key, w_value,
        cache_keys.reshape(seqs, positions * heads, dim),
        cache_values.reshape(seqs, positions * heads, dim),
        lambdas.reshape(1, -1), head_gain.reshape(1, -1), w_out, mlp_gain.reshape(1, -1),
        w_gate.T, w_up.T, w_down,
    )
    vmem = pltpu.VMEM
    local = [vmem(a.shape, a.dtype) for a in args]
    local[-1] = vmem((CHUNKS * 128, 128), BF16)
    tile = (3, 8, 128)
    pair = (6, 8, 128)
    scratch = local + [
        vmem((N_TP, 16, 128), BF16),
        vmem((ROWS, 128), F32),
        vmem((HEADS, *tile), BF16),
        vmem((N_KV, *tile), BF16),
        vmem((HEADS, *pair), BF16),
        vmem((N_KV, *pair), BF16),
        vmem((HEADS, *tile), BF16),
        vmem((2 * HEADS * ROWS, 128), F32),
        vmem((8, 2 * HEADS * ROWS, 128), F32),
        vmem((2 * HEADS * ROWS, 128), F32),
        vmem((HEADS, *pair), BF16),
        vmem((N_KV, *pair), BF16),
        vmem((N_KV, 2, ROWS, 128), F32),
        vmem((N_KV, 2, ROWS, 128), F32),
        vmem((HEADS, *tile), BF16),
        vmem((N_TP, *tile), BF16),
        vmem((N_TP, 16, 128), F32),
        vmem((CHUNKS, *pair), BF16),
        vmem((N_KV, *pair), BF16),
        vmem((CHUNKS, *tile), BF16),
        vmem((N_TP, 16, 128), BF16),
        vmem((N_TP, 16, 128), BF16),
        vmem((seqs, dim, positions * heads), BF16),
        pltpu.SemaphoreType.DMA((len(args),)),
        pltpu.SemaphoreType.DMA((10,)),
        pltpu.SemaphoreType.DMA((10, N_Z)),
    ]
    out = pl.pallas_call(
        kernel,
        out_shape=pltpu.VMEM((tokens.shape[1], seqs), BF16),
        in_specs=[pl.BlockSpec(memory_space=pl.ANY)] * len(args),
        out_specs=pl.BlockSpec(memory_space=pltpu.VMEM),
        scratch_shapes=scratch,
        compiler_params=pltpu.CompilerParams(
            collective_id=0, has_side_effects=True, vmem_limit_bytes=60 * 1024 * 1024
        ),
        name="decode_step",
    )(*args)
    return out.T


def solution(mesh):
    placed = (
        P(None, ("kv", "tp")), P("kv"), P("kv", "tp"), P("kv", "tp"), P("kv", "tp"),
        P(None, "kv", "tp", None), P(None, "kv", "tp", None), P("tp"), P(), P("tp", "kv"),
        P("kv"), P("kv", "tp"), P("kv", "tp"), P("tp", "kv"),
    )
    return jax.shard_map(
        per_device, mesh=mesh, in_specs=placed, out_specs=P(None, ("kv", "tp")), check_vma=False
    )
```

```python
import functools

import jax
import jax.numpy as jnp
from jax import lax
from jax.experimental import pallas as pl
from jax.experimental.pallas import tpu as pltpu
from jax.sharding import PartitionSpec as P

MESH = pl.DeviceIdType.MESH
F32, BF16 = jnp.float32, jnp.bfloat16
D = 4096
EPS = 1e-06
ROWS = 24
SEQS = 22
N_KV, N_X, N_TP = 32, 4, 8
N_Z = N_KV // N_X
KV_ORDER = sorted(
    range(1, N_KV),
    key=lambda i: -(min(i // N_X, N_Z - i // N_X) + min(i % N_X, N_X - i % N_X)),
)
TP_ORDER = (4, 5, 3, 2, 6, 7, 1)
PLANES = sorted(range(N_Z), key=lambda p: min(p, N_Z - p))
HEADS = 4
CHUNKS = 11
LOW = -3.0e38
QUERY_OWNERS = ((0, 8, 16, 24), (6, 14, 22, 30))
HEAD_OWNERS = ((0, 6, 8, 14), (1, 7, 9, 15))
CHUNK_OWNERS = ((0, 2, 5, 8, 11, 14, 17, 20, 23, 26, 29), (1, 3, 6, 9, 12, 15, 18, 21, 24, 27, 30))


def up(block):
    return block.astype(F32).reshape(block.shape[0] * 8, 128)


def tiles(rows):
    return rows.reshape(rows.shape[0] // 8, 8, 128).astype(BF16)


def iota(shape, dim):
    return lax.broadcasted_iota(jnp.int32, shape, dim)


def column_to_row(col):
    shape = (ROWS, 128)
    spread = jnp.where(iota(shape, 0) == iota(shape, 1), jnp.broadcast_to(col, shape), 0.0)
    return jnp.sum(spread, axis=0, keepdims=True)


def row_to_column(row):
    shape = (ROWS, 128)
    spread = jnp.where(iota(shape, 0) == iota(shape, 1), jnp.broadcast_to(row, shape), 0.0)
    return jnp.sum(spread, axis=1, keepdims=True)


def split_two(row):
    high = row.astype(BF16).astype(F32)
    return high, row - high


def with_rows(block, first, second):
    at = iota((ROWS, 128), 0)
    return jnp.where(at == SEQS, first, jnp.where(at == SEQS + 1, second, block))


def kernel(
    tok_hbm, again_hbm, wq_hbm, wk_hbm, wv_hbm, keys_hbm, vals_hbm, lam_hbm, hgain_hbm,
    wo_hbm, mgain_hbm, wg_hbm, wu_hbm, wd_hbm,
    out_ref,
    tok_v, again, wq, wk, wv, keys, vals, lam, hgain, wo, mgain, wg, wu, wd,
    x_all, x_rows,
    b_q, r_q, b_kv, r_kv, q_all, q_s, sc, o_s,
    b_o, r_o, m_s, l_s, h_all, r_b, res_t, b_g, r_g, hid, b_d, r_d,
    keys_t, wg_t, wu_t, load_sem, send_sem, recv_sem,
):
    kv = lax.axis_index("kv")
    tp = lax.axis_index("tp")
    z = kv // N_X
    x = kv % N_X
    core = tp % 2

    def kv_slot(owner):
        return ((z - owner // N_X) % N_Z) * N_X + (x - owner % N_X) % N_X

    def kv_peer(i):
        return ((z + i // N_X) % N_Z) * N_X + (x + i % N_X) % N_X

    def tp_peer(i):
        return (tp + i) % N_TP

    def owner_in(table, n):
        return table[0][n] + (table[1][n] - table[0][n]) * core

    def own_in(table):
        at = [(kv == owner_in(table, n)).astype(jnp.int32) for n in range(len(table[0]))]
        return sum(n * hit for n, hit in enumerate(at)), sum(at) > 0

    query_head, is_query_owner = own_in(QUERY_OWNERS)
    own_head, is_head_owner = own_in(HEAD_OWNERS)
    own_chunk, is_chunk_owner = own_in(CHUNK_OWNERS)

    barrier = pltpu.get_barrier_semaphore()
    for i in range(1, N_TP):
        pl.semaphore_signal(barrier, inc=1, device_id=(kv, tp_peer(i)), device_id_type=MESH)

    for role in (is_query_owner, is_head_owner):

        @pl.when(role)
        def _():
            for i in KV_ORDER:
                pl.semaphore_signal(barrier, inc=1, device_id=(kv_peer(i), tp), device_id_type=MESH)

    loads = [
        pltpu.make_async_copy(src, dst, load_sem.at[n])
        for n, (src, dst) in enumerate(
            (
                (tok_hbm, tok_v), (again_hbm, again), (wq_hbm, wq), (wk_hbm, wk), (wv_hbm, wv),
                (keys_hbm, keys), (vals_hbm, vals), (lam_hbm, lam), (hgain_hbm, hgain),
                (wo_hbm, wo), (mgain_hbm, mgain), (wg_hbm, wg), (wu_hbm, wu),
                (wd_hbm, wd.at[pl.ds(0, wd_hbm.shape[0])]),
            )
        )
    ]
    for load in loads:
        load.start()
    (ld_tok, ld_again, ld_wq, ld_wk, ld_wv, ld_keys, ld_vals, ld_lam, ld_hgain, ld_wo, ld_mgain,
     ld_wg, ld_wu, ld_wd) = loads

    def copy_to(src, dst, phase, device, plane=0):
        return pltpu.make_async_remote_copy(
            src_ref=src, dst_ref=dst, send_sem=send_sem.at[phase],
            recv_sem=recv_sem.at[phase, plane], device_id=device, device_id_type=MESH,
        )

    def plane_slots(ref, phase, p):
        first = 1 if p == 0 else p * N_X
        count = p * N_X + N_X - first
        wait_bytes(ref.at[pl.ds(first, count)], recv_sem.at[phase, p])
        return range(first, first + count)

    def wait_bytes(ref, sem):
        pltpu.make_async_copy(ref, ref, sem).wait()

    wd[pl.ds(wd_hbm.shape[0], CHUNKS * 128 - wd_hbm.shape[0]), :] = jnp.zeros(
        (CHUNKS * 128 - wd_hbm.shape[0], 128), BF16
    )
    b_g[...] = jnp.zeros(b_g.shape, BF16)
    o_s[...] = jnp.zeros(o_s.shape, F32)
    for c in range(8):
        for s in range(SEQS, ROWS):
            sc[c, pl.ds(s, 8, stride=ROWS), :] = jnp.zeros((8, 128), F32)

    ld_tok.wait()
    x_all[tp] = jnp.concatenate(
        [tok_v[...].astype(F32), jnp.zeros((16, 128 - SEQS), F32)], axis=1
    ).astype(BF16)
    own_roles = is_query_owner.astype(jnp.int32) + is_head_owner.astype(jnp.int32)
    pl.semaphore_wait(barrier, N_TP - 1 + 2 * HEADS - own_roles)

    for i in TP_ORDER:
        copy_to(x_all.at[tp], x_all.at[tp], 0, (kv, tp_peer(i))).start()
    ld_again.wait()
    ld_wq.wait()
    wait_bytes(x_all.at[pl.ds(0, N_TP - 1)], recv_sem.at[0, 0])
    x_cols = x_all[...].astype(F32).reshape(128, 128)
    x_f = jnp.transpose(x_cols)[:ROWS]
    x_rows[...] = x_f
    normed = (x_f * again[...]).astype(BF16)
    square_row = column_to_row(jnp.sum(x_f * x_f, axis=1, keepdims=True))
    sq_high, sq_low = split_two(square_row)

    q_part = jnp.dot(normed, wq[...], preferred_element_type=F32)
    for h in range(HEADS):
        b_q[h] = tiles(with_rows(q_part[:, h * 128 : (h + 1) * 128], sq_high, sq_low))
    for h in range(HEADS):
        owner = owner_in(QUERY_OWNERS, h)
        slot = kv_slot(owner)

        @pl.when(owner != kv)
        def _():
            copy_to(b_q.at[h], r_q.at[slot], 1, (owner, tp), slot // N_X).start()

    ld_wk.wait()
    ld_wv.wait()
    k_part = jnp.dot(normed, wk[...], preferred_element_type=F32)
    v_part = jnp.dot(normed, wv[...], preferred_element_type=F32)
    for h in range(HEADS):
        b_kv[h, 0:3] = tiles(with_rows(k_part[:, h * 128 : (h + 1) * 128], sq_high, sq_low))
        b_kv[h, 3:6] = tiles(v_part[:, h * 128 : (h + 1) * 128])
    for h in range(HEADS):
        owner = owner_in(HEAD_OWNERS, h)
        slot = kv_slot(owner)

        @pl.when(owner != kv)
        def _():
            copy_to(b_kv.at[h], r_kv.at[slot], 2, (owner, tp), slot // N_X).start()

    @pl.when(is_query_owner)
    def _():
        total = up(b_q[query_head])
        for p in PLANES:
            for i in plane_slots(r_q, 1, p):
                total = total + up(r_q[i])
        square = total[SEQS : SEQS + 1] + total[SEQS + 1 : SEQS + 2]
        scale = row_to_column(lax.rsqrt(square / D + EPS))
        q_all[query_head] = tiles(scale * total)
        for i in KV_ORDER:
            copy_to(q_all.at[query_head], q_all.at[query_head], 3, (kv_peer(i), tp)).start()

    ld_keys.wait()
    for s in range(SEQS):
        keys_t[s] = jnp.transpose(keys[s])

    role = is_query_owner

    @pl.when(role)
    def _():
        wait_bytes(q_all.at[pl.ds(0, HEADS - 1)], recv_sem.at[3, 0])

    @pl.when(jnp.logical_not(role))
    def _():
        wait_bytes(q_all, recv_sem.at[3, 0])

    lane = iota((ROWS, 128), 1)
    for h in range(HEADS):
        q_h = up(q_all[h]) * 0.125
        q_s[pl.ds((2 * h) * ROWS, ROWS), :] = jnp.where(lane < 64, q_h, 0.0)
        q_s[pl.ds((2 * h + 1) * ROWS, ROWS), :] = jnp.where(lane >= 64, q_h, 0.0)
    for s in range(SEQS):
        q_8 = q_s[pl.ds(s, 8, stride=ROWS), :].astype(BF16)
        part = jnp.dot(q_8, keys_t[s], preferred_element_type=F32)
        for c in range(8):
            sc[c, pl.ds(s, 8, stride=ROWS), :] = part[:, c * 128 : (c + 1) * 128]

    for b in range(2 * HEADS):
        rows = pl.ds(b * ROWS, ROWS)
        mine = (iota((ROWS, 128), 1) % HEADS) == (b // 2)
        top = sc[0, rows, :]
        for c in range(1, 8):
            top = jnp.maximum(top, sc[c, rows, :])
        top = jnp.max(jnp.where(mine, top, LOW), axis=1, keepdims=True)
        total = jnp.zeros((ROWS, 128), F32)
        for c in range(8):
            weight = jnp.where(mine, jnp.exp(jnp.where(mine, sc[c, rows, :], LOW) - top), 0.0)
            sc[c, rows, :] = weight
            total = total + weight
        total = jnp.sum(total, axis=1, keepdims=True)
        m_s[1 + b // 2, b % 2] = jnp.broadcast_to(top, (ROWS, 128))
        l_s[1 + b // 2, b % 2] = jnp.broadcast_to(total, (ROWS, 128))

    ld_vals.wait()
    for s in range(SEQS):
        w_8 = jnp.concatenate(
            [sc[c, pl.ds(s, 8, stride=ROWS), :] for c in range(8)], axis=1
        ).astype(BF16)
        o_s[pl.ds(s, 8, stride=ROWS), :] = jnp.dot(w_8, vals[s], preferred_element_type=F32)

    def stat_row(col_b):
        shape = (ROWS, 128)
        row = jnp.sum(jnp.where(iota(shape, 0) == iota(shape, 1), col_b, 0.0), axis=0, keepdims=True)
        high = row.astype(BF16).astype(F32)
        mid = (row - high).astype(BF16).astype(F32)
        low = (row - high - mid).astype(BF16).astype(F32)
        at = iota((8, 128), 1)
        high, mid, low = (jnp.broadcast_to(v, (8, 128)) for v in (high, mid, low))
        packed = jnp.where(
            at < 32, high, jnp.where(at < 64, pltpu.roll(mid, 32, 1), pltpu.roll(low, 64, 1))
        )
        return packed[0:1]

    for b in range(2 * HEADS):
        h, mp = b // 2, b % 2
        block = with_rows(
            o_s[pl.ds(b * ROWS, ROWS), :], stat_row(m_s[1 + h, mp]), stat_row(l_s[1 + h, mp])
        )
        b_o[h, 3 * mp : 3 * mp + 3] = tiles(block)
    for h in range(HEADS):
        owner = owner_in(HEAD_OWNERS, h)
        slot = kv_slot(owner)

        @pl.when(owner != kv)
        def _():
            copy_to(b_o.at[h], r_o.at[slot], 4, (owner, tp), slot // N_X).start()

    ld_lam.wait()
    ld_hgain.wait()

    @pl.when(is_head_owner)
    def _():
        k_sum = up(b_kv[own_head, 0:3])
        v_sum = up(b_kv[own_head, 3:6])
        for p in PLANES:
            for i in plane_slots(r_kv, 2, p):
                k_sum = k_sum + up(r_kv[i, 0:3])
                v_sum = v_sum + up(r_kv[i, 3:6])
        square = k_sum[SEQS : SEQS + 1] + k_sum[SEQS + 1 : SEQS + 2]
        scale = row_to_column(lax.rsqrt(square / D + EPS))
        k_new = (scale * k_sum).astype(BF16).astype(F32)
        v_new = (scale * v_sum).astype(BF16).astype(F32)
        product = up(q_all[own_head]) * k_new
        r_o[0] = b_o[own_head]
        pieces = iota((ROWS, 128), 1) % 32 == iota((ROWS, 128), 0)
        pieces = jnp.logical_and(pieces, iota((ROWS, 128), 1) < 96)

        def stat_col(row):
            spread = jnp.where(pieces, jnp.broadcast_to(row, (ROWS, 128)), 0.0)
            return jnp.broadcast_to(jnp.sum(spread, axis=1, keepdims=True), (ROWS, 128))

        peak, denom, numer = [], [], []
        for mp in range(2):
            half = jnp.where((lane < 64) == (mp == 0), product, 0.0)
            new = jnp.sum(half, axis=1, keepdims=True) * 0.125
            peak.append(jnp.broadcast_to(new, (ROWS, 128)))
            denom.append(jnp.ones((ROWS, 128), F32))
            numer.append(v_new)
        for p in PLANES:
            slots = list(plane_slots(r_o, 4, p))
            if p == 0:
                slots.append(0)
            for mp in range(2):
                last = [r_o[i, 3 * mp + 2].astype(F32) for i in slots]
                tops = [stat_col(tile[6:7]) for tile in last]
                totals = [stat_col(tile[7:8]) for tile in last]
                above = functools.reduce(jnp.maximum, tops, peak[mp])
                fade = jnp.exp(peak[mp] - above)
                n, d = numer[mp] * fade, denom[mp] * fade
                for i, top, total in zip(slots, tops, totals):
                    weight = jnp.exp(top - above)
                    n = n + weight * up(r_o[i, 3 * mp : 3 * mp + 3])
                    d = d + weight * total
                peak[mp], numer[mp], denom[mp] = above, n, d
        results = [numer[mp] / denom[mp] for mp in range(2)]
        mine = iota((1, HEADS), 1) == own_head
        lam_h = jnp.sum(jnp.where(mine, lam[...], 0.0), axis=1, keepdims=True)
        difference = results[0] - lam_h * results[1]
        mean = jnp.mean(difference * difference, axis=1, keepdims=True)
        h_all[own_head] = tiles(difference * lax.rsqrt(mean + EPS) * hgain[...])
        for i in KV_ORDER:
            copy_to(h_all.at[own_head], h_all.at[own_head], 5, (kv_peer(i), tp)).start()

    ld_wg.wait()
    ld_wu.wait()
    width = wg.shape[0]
    for j in range(CHUNKS):
        lo, hi = j * 128, min(j * 128 + 128, width)
        wg_t[j, :, 0 : hi - lo] = jnp.transpose(wg[lo:hi, :])
        wu_t[j, :, 0 : hi - lo] = jnp.transpose(wu[lo:hi, :])

    @pl.when(is_head_owner)
    def _():
        wait_bytes(h_all.at[pl.ds(0, HEADS - 1)], recv_sem.at[5, 0])

    @pl.when(jnp.logical_not(is_head_owner))
    def _():
        wait_bytes(h_all, recv_sem.at[5, 0])

    ld_wo.wait()
    heads_out = jnp.concatenate([up(h_all[h]) for h in range(HEADS)], axis=1).astype(BF16)
    r_b[tp] = tiles(jnp.dot(heads_out, wo[...], preferred_element_type=F32))
    for i in TP_ORDER:
        copy_to(r_b.at[tp], r_b.at[tp], 6, (kv, tp_peer(i))).start()
    ld_mgain.wait()
    wait_bytes(r_b.at[pl.ds(0, N_TP - 1)], recv_sem.at[6, 0])
    branch = up(r_b[0])
    for i in range(1, N_TP):
        branch = branch + up(r_b[i])
    live = iota((ROWS, 128), 0) < SEQS
    residual = jnp.where(live, (x_rows[...] + branch).astype(BF16).astype(F32), 0.0)
    normed_mid = (residual * mgain[...]).astype(BF16)
    sq_high, sq_low = split_two(
        column_to_row(jnp.sum(residual * residual, axis=1, keepdims=True))
    )

    for j in range(CHUNKS):
        lo, hi = j * 128, min(j * 128 + 128, width)
        n = hi - lo
        at = iota((ROWS, n), 0)
        g_j = jnp.dot(normed_mid, wg_t[j, :, 0:n], preferred_element_type=F32)
        u_j = jnp.dot(normed_mid, wu_t[j, :, 0:n], preferred_element_type=F32)
        g_j = jnp.where(at == SEQS, sq_high[:, :n], jnp.where(at == SEQS + 1, sq_low[:, :n], g_j))
        b_g[j, 0:3, :, 0:n] = g_j.reshape(3, 8, n).astype(BF16)
        b_g[j, 3:6, :, 0:n] = u_j.reshape(3, 8, n).astype(BF16)
        owner = owner_in(CHUNK_OWNERS, j)
        slot = kv_slot(owner)

        @pl.when(owner != kv)
        def _():
            copy_to(b_g.at[j], r_g.at[slot], 7, (owner, tp), slot // N_X).start()

    res_t[...] = jnp.transpose(
        jnp.concatenate([residual, jnp.zeros((128 - ROWS, 128), F32)], axis=0)
    ).reshape(N_TP, 16, 128)

    @pl.when(is_chunk_owner)
    def _():
        gate = up(b_g[own_chunk, 0:3])
        upper = up(b_g[own_chunk, 3:6])
        for p in PLANES:
            for i in plane_slots(r_g, 7, p):
                gate = gate + up(r_g[i, 0:3])
                upper = upper + up(r_g[i, 3:6])
        square = gate[SEQS : SEQS + 1] + gate[SEQS + 1 : SEQS + 2]
        scale = row_to_column(lax.rsqrt(square / D + EPS))
        gate = scale * gate
        hidden = (gate / (1.0 + jnp.exp(-gate))) * (scale * upper)
        hid[own_chunk] = tiles(hidden)
        for i in KV_ORDER:
            copy_to(hid.at[own_chunk], hid.at[own_chunk], 8, (kv_peer(i), tp)).start()
        wait_bytes(hid.at[pl.ds(0, CHUNKS - 1)], recv_sem.at[8, 0])

    @pl.when(jnp.logical_not(is_chunk_owner))
    def _():
        wait_bytes(hid, recv_sem.at[8, 0])

    ld_wd.wait()
    hidden_all = jnp.concatenate([up(hid[j]) for j in range(CHUNKS)], axis=1).astype(BF16)
    down = jnp.dot(hidden_all, wd[...], preferred_element_type=F32)
    down_t = jnp.transpose(
        jnp.concatenate([down, jnp.zeros((128 - ROWS, 128), F32)], axis=0)
    )
    b_d[...] = down_t.reshape(N_TP, 16, 128).astype(BF16)
    r_d[tp] = b_d[tp]
    for i in TP_ORDER:
        peer = tp_peer(i)
        copy_to(b_d.at[peer], r_d.at[tp], 9, (kv, peer)).start()
    wait_bytes(r_d.at[pl.ds(0, N_TP - 1)], recv_sem.at[9, 0])
    mixer = r_d[0].astype(F32)
    for i in range(1, N_TP):
        mixer = mixer + r_d[i].astype(F32)
    out_ref[...] = (res_t[tp] + mixer).astype(BF16)[:, :SEQS]

    wait_bytes(x_all.at[pl.ds(0, N_TP - 1)], send_sem.at[0])
    wait_bytes(r_b.at[pl.ds(0, N_TP - 1)], send_sem.at[6])
    wait_bytes(r_d.at[pl.ds(0, N_TP - 1)], send_sem.at[9])

    @pl.when(is_query_owner)
    def _():
        wait_bytes(r_q.at[pl.ds(0, HEADS - 1)], send_sem.at[1])
        wait_bytes(r_q.at[pl.ds(1, N_KV - 1)], send_sem.at[3])

    @pl.when(jnp.logical_not(is_query_owner))
    def _():
        wait_bytes(r_q.at[pl.ds(0, HEADS)], send_sem.at[1])

    @pl.when(is_head_owner)
    def _():
        wait_bytes(r_kv.at[pl.ds(0, HEADS - 1)], send_sem.at[2])
        wait_bytes(r_o.at[pl.ds(0, HEADS - 1)], send_sem.at[4])
        wait_bytes(r_q.at[pl.ds(1, N_KV - 1)], send_sem.at[5])

    @pl.when(jnp.logical_not(is_head_owner))
    def _():
        wait_bytes(r_kv.at[pl.ds(0, HEADS)], send_sem.at[2])
        wait_bytes(r_o.at[pl.ds(0, HEADS)], send_sem.at[4])

    @pl.when(is_chunk_owner)
    def _():
        wait_bytes(r_g.at[pl.ds(0, CHUNKS - 1)], send_sem.at[7])
        wait_bytes(r_q.at[pl.ds(1, N_KV - 1)], send_sem.at[8])

    @pl.when(jnp.logical_not(is_chunk_owner))
    def _():
        wait_bytes(r_g.at[pl.ds(0, CHUNKS)], send_sem.at[7])


def per_device(
    tokens, attn_gain, w_query, w_key, w_value, cache_keys, cache_values, lambdas, head_gain,
    w_out, mlp_gain, w_gate, w_up, w_down,
):
    seqs, positions, heads, dim = cache_keys.shape
    args = (
        tokens.T, attn_gain.reshape(1, -1), w_query, w_key, w_value,
        cache_keys.reshape(seqs, positions * heads, dim),
        cache_values.reshape(seqs, positions * heads, dim),
        lambdas.reshape(1, -1), head_gain.reshape(1, -1), w_out, mlp_gain.reshape(1, -1),
        w_gate.T, w_up.T, w_down,
    )
    vmem = pltpu.VMEM
    local = [vmem(a.shape, a.dtype) for a in args]
    local[-1] = vmem((CHUNKS * 128, 128), BF16)
    tile = (3, 8, 128)
    pair = (6, 8, 128)
    scratch = local + [
        vmem((N_TP, 16, 128), BF16),
        vmem((ROWS, 128), F32),
        vmem((HEADS, *tile), BF16),
        vmem((N_KV, *tile), BF16),
        vmem((HEADS, *pair), BF16),
        vmem((N_KV, *pair), BF16),
        vmem((HEADS, *tile), BF16),
        vmem((2 * HEADS * ROWS, 128), F32),
        vmem((8, 2 * HEADS * ROWS, 128), F32),
        vmem((2 * HEADS * ROWS, 128), F32),
        vmem((HEADS, *pair), BF16),
        vmem((N_KV, *pair), BF16),
        vmem((N_KV, 2, ROWS, 128), F32),
        vmem((N_KV, 2, ROWS, 128), F32),
        vmem((HEADS, *tile), BF16),
        vmem((N_TP, *tile), BF16),
        vmem((N_TP, 16, 128), F32),
        vmem((CHUNKS, *pair), BF16),
        vmem((N_KV, *pair), BF16),
        vmem((CHUNKS, *tile), BF16),
        vmem((N_TP, 16, 128), BF16),
        vmem((N_TP, 16, 128), BF16),
        vmem((seqs, dim, positions * heads), BF16),
        vmem((CHUNKS, 128, 128), BF16),
        vmem((CHUNKS, 128, 128), BF16),
        pltpu.SemaphoreType.DMA((len(args),)),
        pltpu.SemaphoreType.DMA((10,)),
        pltpu.SemaphoreType.DMA((10, N_Z)),
    ]
    out = pl.pallas_call(
        kernel,
        out_shape=pltpu.VMEM((tokens.shape[1], seqs), BF16),
        in_specs=[pl.BlockSpec(memory_space=pl.ANY)] * len(args),
        out_specs=pl.BlockSpec(memory_space=pltpu.VMEM),
        scratch_shapes=scratch,
        compiler_params=pltpu.CompilerParams(
            collective_id=0, has_side_effects=True, vmem_limit_bytes=60 * 1024 * 1024
        ),
        name="decode_step",
    )(*args)
    return out.T


def solution(mesh):
    placed = (
        P(None, ("kv", "tp")), P("kv"), P("kv", "tp"), P("kv", "tp"), P("kv", "tp"),
        P(None, "kv", "tp", None), P(None, "kv", "tp", None), P("tp"), P(), P("tp", "kv"),
        P("kv"), P("kv", "tp"), P("kv", "tp"), P("tp", "kv"),
    )
    return jax.shard_map(
        per_device, mesh=mesh, in_specs=placed, out_specs=P(None, ("kv", "tp")), check_vma=False
    )
```
